32 devices in a mesh: sp: 8 (over z, x), tp: 4 (over y, core).
Axes of the slice: x: 2, y: 2, z: 4, core: 2. Of those that a mesh axis runs over, the one named last changes fastest.
Arguments:
- moe_input: bfloat16 [2048, 2048], P('sp'), may hold values from -6 to 6
- out_cotangent: bfloat16 [2048, 2048], P('sp'), may hold values from -6 to 6
- routes: int32 [2048, 2], P('sp'), may hold values from 0 to 7, all different within a row; in each aligned block of 256 rows (0 to 255, 256 to 511, ...) at most 96 rows name the same one
- group_weight: float32 [2048], P('sp'), may hold values from 0.5 to 1
- inner_weight: float32 [2048, 2], P('sp'), may hold values from 0.3 to 1
- gate_weight: bfloat16 [8, 2048, 1024], P('sp', None, 'tp'), may hold values from -0.125 to 0.125
- up_weight: bfloat16 [8, 2048, 1024], P('sp', None, 'tp'), may hold values from -0.125 to 0.125
- down_weight: bfloat16 [8, 1024, 2048], P('sp', 'tp'), may hold values from -0.1875 to 0.1875
- value_in: bfloat16 [2048, 1024], P('sp', 'tp'), may hold values from -6 to 6
- gate_in: bfloat16 [2048, 1024], P('sp', 'tp'), may hold values from -6 to 6
- conv_taps: bfloat16 [31, 1024], P(None, 'tp'), may hold values from -1 to 1
- norm_hat: bfloat16 [2048, 1024], P('sp', 'tp'), may hold values from -6 to 6
- norm_rstd: float32 [2048], P('sp'), may hold values from 0.3 to 3
- norm_gain: float32 [1024], P('tp'), may hold values from 0.1 to 1.9
- out_proj: bfloat16 [2048, 1024], P(None, 'tp'), may hold values from -0.1875 to 0.1875
Outputs:
- gate_grad: bfloat16 [8, 2048, 1024], P('sp', None, 'tp')
- up_grad: bfloat16 [8, 2048, 1024], P('sp', None, 'tp')
- down_grad: bfloat16 [8, 1024, 2048], P('sp', 'tp')
- proj_grad: float32 [2048, 1024], P('sp', 'tp')
- value_grad: bfloat16 [2048, 1024], P('sp', 'tp')
- gate_in_grad: bfloat16 [2048, 1024], P('sp', 'tp')
The draws below stay inside these ranges and needn't reach their ends.
Inputs may be any that keep to these rules, and one draw needn't show every extreme that they name: In the rows of one device (aligned blocks of 256 tokens) no expert is named by more than 96 routes, and in every draw some expert is named by exactly 96 in some block; a token's two experts differ.
All inputs are finite; a program needn't handle non-finite values.
Results may differ from the reference program's by a relative error of at most 0.009.
Values may be sent and summed in bfloat16 or wider, within the bound.
A program may use at most 128 MiB of HBM per device.

```python
import math
import jax
import jax.numpy as jnp
import numpy as np
from jax import lax

D = 2048
CONV = 1024
FF = 1024
KERNEL = 31
TOK_DEV = 256
EXPERTS = 8
CAP = 96
TOKENS = 2048
N_TP = 4


def raised(array, own_key, source, target, blocks, factor):
    owner, partner = [(jnp.arange(array.shape[axis_at]) // (array.shape[axis_at] // blocks)).reshape([-1 if axis == axis_at else 1 for axis in range(array.ndim)]) for axis_at in (source, target)]
    chosen = jax.random.permutation(own_key, blocks)[partner]
    strong = (owner == chosen) | (owner == (partner + blocks // 2) % blocks)
    return jnp.where(strong, factor * array, array)


def steps_of(own_key, extent, split, smallest, largest):
    level = 1.0
    for axis_at, shards_of in split:
        steps = jax.random.uniform(jax.random.fold_in(jax.random.fold_in(own_key, 6), axis_at), (shards_of,), jnp.float32, smallest / len(split), largest / len(split))
        level = level * jnp.repeat(jnp.exp(steps), extent[axis_at] // shards_of).reshape((-1,) + (1,) * (len(extent) - 1 - axis_at))
    return level


def deal_out(key, own, number, rows, number_of, top, most, lean):
    sequence = jax.random.permutation(key, number_of)
    crowded, common = shares(number_of, rows * top, most, lean, True), shares(number_of, rows * top, most, lean, False)
    places = jnp.arange(number_of)

    def named(sizes, rotation):
        used = int((sizes > 0).sum())
        fixed = max(1, used // 4)
        passed = fixed + (places - fixed + rotation * (used - fixed)) % max(1, number_of - fixed)
        return jnp.zeros((number_of,), jnp.int32).at[sequence[jnp.where(places < fixed, places, passed)]].set(jnp.asarray(sizes, jnp.int32))

    sizes = jnp.where(number % 4 == 0, named(crowded, number // 4), named(common, number - number // 4 - 1))
    mixed = jax.random.permutation(jax.random.fold_in(own, 3), number_of)
    source_of, sink = mixed[0:number_of // 2 * 2:2], mixed[1:number_of // 2 * 2:2]
    room = jnp.minimum(sizes[source_of] - 1, most - sizes[sink]) // 2
    room = jnp.where((source_of == sequence[0]) | (sink == sequence[0]) | (sizes[sink] == 0), 0, jnp.maximum(room, 0))
    passed = jax.random.randint(jax.random.fold_in(own, 4), (number_of // 2,), 0, 1 << 20) % (room + 1)
    sizes = sizes.at[source_of].add(-passed).at[sink].add(passed)
    items = jnp.searchsorted(jnp.cumsum(sizes), jnp.arange(rows * top), side="right").astype(jnp.int32)
    grid = items.reshape(top, rows).T
    grid = grid[jax.random.permutation(jax.random.fold_in(own, 1), rows)]
    rotation = jax.random.randint(jax.random.fold_in(own, 2), (rows, 1), 0, top)
    return jnp.take_along_axis(grid, (jnp.arange(top)[None, :] + rotation) % top, axis=1)


def shares(number_of, total, limit, slope, full):
    weights = [(1 << 20) // math.isqrt(grade ** slope) + 1 for grade in range(1, number_of + 1)]
    largest = limit if full else min(limit, max(-(-total // number_of), total * weights[0] // sum(weights)))
    least = 1 if total - largest >= number_of - 1 else 0
    counts, surplus = [largest] + [least] * (number_of - 1), total - largest - least * (number_of - 1)
    while surplus > 0:
        candidates = [i for i in range(1, number_of) if counts[i] < largest] or [i for i in range(1, number_of) if counts[i] < limit]
        pool, left = sum([weights[i] for i in candidates]), surplus
        for i in candidates:
            extra = min(limit - counts[i], max(1, left * weights[i] // pool), surplus)
            counts[i] = counts[i] + extra
            surplus = surplus - extra
    return np.array(counts)


def noise(stream_key, dims, spread, limit, split=(), kind=jnp.bfloat16):
    values = spread * jax.random.normal(stream_key, dims, jnp.float32)
    if split:
        values = values * steps_of(stream_key, dims, split, -0.22, 0.18)
    return jnp.clip(values, -limit, limit).astype(kind)


def gaussian_with(rng, dims, deviation, limit, shards, heavy, kind=jnp.bfloat16):
    drawn = deviation * jax.random.normal(rng, dims, jnp.float32)
    if shards:
        drawn = drawn * steps_of(rng, dims, shards, -0.22, 0.18)
    return jnp.clip(raised(drawn, jax.random.fold_in(rng, 3), *heavy), -limit, limit).astype(kind)


def setup_inputs(seed: int = 0) -> dict:
    seeds = jax.random.split(jax.random.key(seed), 16)
    moe_input = noise(seeds[0], (TOKENS, D), 1.0, 6.0, ((0, 8),))
    out_cotangent = gaussian_with(seeds[1], (TOKENS, D), 1.0, 6.0, ((0, 8),), (0, 1, 8, 2.0))
    routes_keys = jax.random.split(jax.random.fold_in(seeds[2], 1), TOKENS // TOK_DEV)
    routes_turns = jax.random.permutation(jax.random.fold_in(seeds[2], 3), TOKENS // TOK_DEV)
    routes = jax.vmap(lambda own, number: deal_out(jax.random.fold_in(seeds[2], 2), own, number, TOK_DEV, EXPERTS, 2, CAP, 2))(routes_keys, routes_turns).reshape((TOKENS, 2))
    group_weight = jnp.clip(0.5 + 0.5 * jax.random.uniform(seeds[3], (TOKENS,), jnp.float32) ** steps_of(seeds[3], (TOKENS,), ((0, 8),), -0.2, 0.2), 0.5, 1.0)
    inner_weight = jnp.clip(0.3 + 0.7 * jax.random.uniform(seeds[4], (TOKENS, 2), jnp.float32) ** steps_of(seeds[4], (TOKENS, 2), ((0, 8),), -0.2, 0.2), 0.3, 1.0)
    gate_weight = noise(seeds[5], (EXPERTS, D, FF), D ** -0.5, 0.125, ((0, 8), (2, 4)))
    up_weight = noise(seeds[6], (EXPERTS, D, FF), D ** -0.5, 0.125, ((0, 8), (2, 4)))
    down_weight = noise(seeds[7], (EXPERTS, FF, D), FF ** -0.5, 0.1875, ((0, 8), (1, 4)))
    value_in = noise(seeds[8], (TOKENS, CONV), 1.0, 6.0, ((0, 8), (1, 4)))
    gate_in = noise(seeds[9], (TOKENS, CONV), 1.0, 6.0, ((0, 8), (1, 4)))
    conv_taps = noise(seeds[10], (KERNEL, CONV), KERNEL ** -0.5, 1.0, ((1, 4),))
    norm_hat = noise(seeds[11], (TOKENS, CONV), 1.0, 6.0, ((0, 8), (1, 4)))
    norm_rstd = jnp.clip(jnp.exp(math.log(3.0) - 2.3025851 * jax.random.uniform(seeds[12], (TOKENS,), jnp.float32) ** steps_of(seeds[12], (TOKENS,), ((0, 8),), -0.2, 0.2)), 0.3, 3.0)
    norm_gain = jnp.clip(1.0 + 0.18 * jax.random.normal(seeds[13], (CONV,), jnp.float32), 0.1, 1.9)
    out_proj = noise(seeds[14], (D, CONV), CONV ** -0.5, 0.1875, ((1, 4),))
    return dict(moe_input=moe_input, out_cotangent=out_cotangent, routes=routes, group_weight=group_weight, inner_weight=inner_weight, gate_weight=gate_weight, up_weight=up_weight, down_weight=down_weight, value_in=value_in, gate_in=gate_in, conv_taps=conv_taps, norm_hat=norm_hat, norm_rstd=norm_rstd, norm_gain=norm_gain, out_proj=out_proj)


def round_half(values):
    return lax.optimization_barrier(values.astype(jnp.bfloat16)).astype(jnp.float32)


def silu_slope(logits, squashed):
    return squashed * (1.0 + logits * (1.0 - squashed))


def reference(moe_input, out_cotangent, routes, group_weight, inner_weight, gate_weight, up_weight, down_weight, value_in, gate_in, conv_taps, norm_hat, norm_rstd, norm_gain, out_proj):
    tok_total, model_width = moe_input.shape
    all_experts = gate_weight.shape[0]
    hidden_units = gate_weight.shape[2]
    block_count = tok_total // TOK_DEV
    block_routes = 2 * TOK_DEV
    total_routes = 2 * tok_total
    routes_flat = routes.reshape(block_count, block_routes).astype(jnp.int32)
    one_hot = (routes_flat[:, :, None] == jnp.arange(all_experts, dtype=jnp.int32)[None, None, :]).astype(jnp.int32)
    slot_rank = jnp.sum(one_hot * (jnp.cumsum(one_hot, axis=1) - one_hot), axis=2)
    expert_rows = block_count * CAP
    slot_index = routes_flat * expert_rows + jnp.arange(block_count, dtype=jnp.int32)[:, None] * CAP + slot_rank
    slot_index = slot_index.reshape(total_routes).astype(jnp.int32)
    slot_owner = jnp.full((all_experts * expert_rows,), total_routes, jnp.int32).at[slot_index].set(jnp.arange(total_routes, dtype=jnp.int32))
    route_weight = group_weight[:, None] * inner_weight
    scaled = (route_weight[:, :, None] * out_cotangent.astype(jnp.float32)[:, None, :]).astype(jnp.bfloat16)
    scaled = jnp.concatenate([scaled.reshape(total_routes, model_width), jnp.zeros((1, model_width), jnp.bfloat16)])
    inputs = jnp.concatenate([moe_input, jnp.zeros((1, model_width), jnp.bfloat16)])
    owners = slot_owner.reshape(all_experts, expert_rows)
    quarter = hidden_units // N_TP

    def one_expert(packed):
        w_gate, w_up, w_down, members = packed
        slot_grad = scaled[members]
        slot_input = inputs[members // 2]
        gate_pre = jnp.dot(slot_input, w_gate, preferred_element_type=jnp.float32)
        up_pre = jnp.dot(slot_input, w_up, preferred_element_type=jnp.float32)
        gate_sigma = jax.nn.sigmoid(gate_pre)
        hidden_act = (gate_pre * gate_sigma * up_pre).astype(jnp.bfloat16)
        act_grad = jnp.dot(slot_grad, w_down.T, preferred_element_type=jnp.float32)
        gate_delta = (act_grad * up_pre * silu_slope(gate_pre, gate_sigma)).astype(jnp.bfloat16)
        up_delta = (act_grad * gate_pre * gate_sigma).astype(jnp.bfloat16)
        down_part = jnp.dot(hidden_act.T, slot_grad, preferred_element_type=jnp.float32).astype(jnp.bfloat16)
        gate_part = jnp.dot(slot_input.T, gate_delta, preferred_element_type=jnp.float32).astype(jnp.bfloat16)
        up_part = jnp.dot(slot_input.T, up_delta, preferred_element_type=jnp.float32).astype(jnp.bfloat16)
        summed = jnp.zeros((members.shape[0], model_width), jnp.float32)
        for block in range(N_TP):
            lower = block * quarter
            upper = lower + quarter
            partial_value = jnp.dot(gate_delta[:, lower:upper], w_gate[:, lower:upper].T, preferred_element_type=jnp.float32)
            partial_value = partial_value + jnp.dot(up_delta[:, lower:upper], w_up[:, lower:upper].T, preferred_element_type=jnp.float32)
            summed = summed + round_half(partial_value)
        return gate_part, up_part, down_part, summed.astype(jnp.bfloat16)

    gate_grad, up_grad, down_grad, slot_back = lax.map(one_expert, (gate_weight, up_weight, down_weight, owners))
    route_back = slot_back.reshape(all_experts * expert_rows, model_width)[slot_index]
    returned = jnp.sum(route_back.reshape(tok_total, 2, model_width).astype(jnp.float32), axis=1)
    mixer_grad = (out_cotangent.astype(jnp.float32) + returned).astype(jnp.bfloat16)
    normed = norm_hat.astype(jnp.float32) * norm_gain[None, :]
    norm_sigma = jax.nn.sigmoid(normed)
    mixer_act = (normed * norm_sigma).astype(jnp.bfloat16)
    proj_grad = jnp.dot(mixer_grad.T, mixer_act, preferred_element_type=jnp.float32)
    silu_grad = jnp.dot(mixer_grad, out_proj, preferred_element_type=jnp.float32)
    hat_grad = silu_grad * silu_slope(normed, norm_sigma) * norm_gain[None, :]
    norm_values = norm_hat.astype(jnp.float32)
    grad_mean = jnp.mean(hat_grad, axis=1, keepdims=True)
    grad_dot = jnp.mean(hat_grad * norm_values, axis=1, keepdims=True)
    conv_grad = norm_rstd[:, None] * (hat_grad - grad_mean - norm_values * grad_dot)
    tap_count = conv_taps.shape[0]
    extended = jnp.pad(conv_grad, ((0, tap_count - 1), (0, 0)))
    tap_values = conv_taps.astype(jnp.float32)
    glu_grad = jnp.zeros_like(conv_grad)
    for offset in range(tap_count):
        lower = tap_count - 1 - offset
        glu_grad = glu_grad + tap_values[offset][None, :] * extended[lower:lower + tok_total]
    gate_sigma = jax.nn.sigmoid(gate_in.astype(jnp.float32))
    value_grad = (glu_grad * gate_sigma).astype(jnp.bfloat16)
    gate_in_grad = (glu_grad * value_in.astype(jnp.float32) * gate_sigma * (1.0 - gate_sigma)).astype(jnp.bfloat16)
    return gate_grad, up_grad, down_grad, proj_grad, value_grad, gate_in_grad
```

```python
import functools

import jax
import jax.numpy as jnp
from jax import lax
from jax.experimental import pallas as pl
from jax.experimental.pallas import tpu as pltpu
from jax.sharding import PartitionSpec as P


def shifted(block, axis, distance):
    devices = range(lax.axis_size(axis))
    route = [(i - distance, i) for i in devices if i - distance in devices]
    return lax.ppermute(block, axis, route)


def silu_slope(logits, squashed):
    return squashed * (1.0 + logits * (1.0 - squashed))


def by_collectives(
    moe_input,
    out_cotangent,
    routes,
    group_weight,
    inner_weight,
    gate_weight,
    up_weight,
    down_weight,
    value_in,
    gate_in,
    conv_taps,
    norm_hat,
    norm_rstd,
    norm_gain,
    out_proj,
):
    tok_rows, model_width = moe_input.shape
    local_experts = gate_weight.shape[0]
    sp_count = lax.axis_size("sp")
    tp_count = lax.axis_size("tp")
    all_experts = local_experts * sp_count
    capacity = 3 * tok_rows // all_experts
    col_width = model_width // tp_count
    col_start = lax.axis_index("tp") * col_width
    route_count = 2 * tok_rows
    routes_flat = routes.reshape(route_count)
    one_hot = (routes_flat[:, None] == jnp.arange(all_experts, dtype=jnp.int32)[None, :]).astype(
        jnp.int32
    )
    slot_rank = jnp.sum(one_hot * (jnp.cumsum(one_hot, axis=0) - one_hot), axis=1)
    slot_index = routes_flat * capacity + slot_rank
    slot_owner = (
        jnp.full((all_experts * capacity,), route_count, jnp.int32)
        .at[slot_index]
        .set(jnp.arange(route_count, dtype=jnp.int32))
    )
    route_weight = (group_weight[:, None] * inner_weight).reshape(route_count)
    slot_weight = jnp.concatenate([route_weight, jnp.zeros((1,), jnp.float32)])[slot_owner]
    slot_token = slot_owner // 2
    grad_cols = lax.dynamic_slice_in_dim(out_cotangent, col_start, col_width, 1)
    input_cols = lax.dynamic_slice_in_dim(moe_input, col_start, col_width, 1)
    zero_row = jnp.zeros((1, grad_cols.shape[1]), grad_cols.dtype)
    padded_grad = jnp.concatenate([grad_cols, zero_row])[slot_token]
    padded_input = jnp.concatenate([input_cols, zero_row])[slot_token]
    scaled = (slot_weight[:, None] * padded_grad.astype(jnp.float32)).astype(jnp.bfloat16)
    slot_shape = (sp_count, local_experts * capacity, grad_cols.shape[1])
    arrived = (
        lax.all_to_all(scaled.reshape(slot_shape), "sp", split_axis=0, concat_axis=0, tiled=True),
        lax.all_to_all(
            padded_input.reshape(slot_shape), "sp", split_axis=0, concat_axis=0, tiled=True
        ),
    )
    slot_grad, slot_input = (
        lax.all_gather(arrived[0], "tp", axis=2, tiled=True),
        lax.all_gather(arrived[1], "tp", axis=2, tiled=True),
    )

    def by_expert(slot_rows):
        return (
            slot_rows.reshape(sp_count, local_experts, capacity, model_width)
            .transpose(1, 0, 2, 3)
            .reshape(local_experts, sp_count * capacity, model_width)
        )

    expert_grad = by_expert(slot_grad)
    expert_input = by_expert(slot_input)
    gate_pre = jnp.einsum(
        "emd,edf->emf", expert_input, gate_weight, preferred_element_type=jnp.float32
    )
    up_pre = jnp.einsum("emd,edf->emf", expert_input, up_weight, preferred_element_type=jnp.float32)
    gate_sigma = jax.nn.sigmoid(gate_pre)
    hidden_act = (gate_pre * gate_sigma * up_pre).astype(jnp.bfloat16)
    act_grad = jnp.einsum(
        "emd,efd->emf", expert_grad, down_weight, preferred_element_type=jnp.float32
    )
    gate_delta = (act_grad * up_pre * silu_slope(gate_pre, gate_sigma)).astype(jnp.bfloat16)
    up_delta = (act_grad * gate_pre * gate_sigma).astype(jnp.bfloat16)
    down_grad = jnp.einsum(
        "emf,emd->efd", hidden_act, expert_grad, preferred_element_type=jnp.float32
    ).astype(jnp.bfloat16)
    gate_grad = jnp.einsum(
        "emd,emf->edf", expert_input, gate_delta, preferred_element_type=jnp.float32
    ).astype(jnp.bfloat16)
    up_grad = jnp.einsum(
        "emd,emf->edf", expert_input, up_delta, preferred_element_type=jnp.float32
    ).astype(jnp.bfloat16)
    partial_value = jnp.einsum(
        "emf,edf->emd", gate_delta, gate_weight, preferred_element_type=jnp.float32
    )
    partial_value = partial_value + jnp.einsum(
        "emf,edf->emd", up_delta, up_weight, preferred_element_type=jnp.float32
    )
    summed = lax.psum_scatter(
        partial_value.astype(jnp.bfloat16).astype(jnp.float32).astype(jnp.bfloat16),
        "tp",
        scatter_dimension=2,
        tiled=True,
    )
    returned = summed.reshape(local_experts, sp_count, capacity, col_width)
    returned = returned.transpose(1, 0, 2, 3).reshape(sp_count, local_experts * capacity, col_width)
    arrived_back = lax.all_to_all(returned, "sp", split_axis=0, concat_axis=0, tiled=True)
    route_grad = arrived_back.reshape(all_experts * capacity, col_width)[slot_index].astype(
        jnp.float32
    )
    mixed_cols = jnp.sum(route_grad.reshape(tok_rows, 2, col_width), axis=1)
    own_cols = lax.dynamic_slice_in_dim(out_cotangent, col_start, col_width, 1).astype(jnp.float32)
    mixer_part = (own_cols + mixed_cols).astype(jnp.bfloat16)
    mixer_grad = lax.all_gather(mixer_part, "tp", axis=1, tiled=True)
    normed = norm_hat.astype(jnp.float32) * norm_gain[None, :]
    norm_sigma = jax.nn.sigmoid(normed)
    mixer_act = (normed * norm_sigma).astype(jnp.bfloat16)
    proj_grad = lax.psum_scatter(
        jnp.einsum("tc,tk->ck", mixer_grad, mixer_act, preferred_element_type=jnp.float32),
        "sp",
        scatter_dimension=0,
        tiled=True,
    )
    silu_grad = jnp.dot(mixer_grad, out_proj, preferred_element_type=jnp.float32)
    hat_grad = silu_grad * silu_slope(normed, norm_sigma) * norm_gain[None, :]
    norm_values = norm_hat.astype(jnp.float32)
    grad_sum, grad_dot = lax.psum(
        (jnp.sum(hat_grad, axis=1), jnp.sum(hat_grad * norm_values, axis=1)), "tp"
    )
    channels = norm_values.shape[1] * tp_count
    conv_grad = norm_rstd[:, None] * (
        hat_grad - grad_sum[:, None] / channels - norm_values * (grad_dot[:, None] / channels)
    )
    tap_count = conv_taps.shape[0]
    incoming = shifted(conv_grad[: tap_count - 1], "sp", -1)
    extended = jnp.concatenate([conv_grad, incoming], axis=0)
    tap_values = conv_taps.astype(jnp.float32)
    glu_grad = jnp.zeros_like(conv_grad)
    for offset in range(tap_count):
        lower = tap_count - 1 - offset
        glu_grad = glu_grad + tap_values[offset][None, :] * extended[lower : lower + tok_rows]
    input_sigma = jax.nn.sigmoid(gate_in.astype(jnp.float32))
    value_grad = (glu_grad * input_sigma).astype(jnp.bfloat16)
    gate_in_grad = (
        glu_grad * value_in.astype(jnp.float32) * input_sigma * (1.0 - input_sigma)
    ).astype(jnp.bfloat16)
    return (gate_grad, up_grad, down_grad, proj_grad, value_grad, gate_in_grad)


MESH = pl.DeviceIdType.MESH


def remote(src, dst, send_sem, recv_sem, device):
    return pltpu.make_async_remote_copy(
        src_ref=src,
        dst_ref=dst,
        send_sem=send_sem,
        recv_sem=recv_sem,
        device_id=device,
        device_id_type=MESH,
    )


def greet(devices):
    barrier = pltpu.get_barrier_semaphore()
    for device in devices:
        pl.semaphore_signal(barrier, inc=1, device_id=device, device_id_type=MESH)
    pl.semaphore_wait(barrier, len(devices))


def rows_of(block, rows):
    return pl.ds(pl.multiple_of(block * rows, rows), rows)


def ring_peers(sp_count):
    me = lax.axis_index("sp")
    partners = [me]
    for mask in range(sp_count - 1, 0, -1):
        partner, bit = 0, 1
        while bit < sp_count:
            partner = partner + bit * (((me // bit) + (mask // bit)) % 2)
            bit = 2 * bit
        partners.append(partner)
    return me, partners, partners


def tp_places():
    t = lax.axis_index("tp")
    pair = t // 2
    core = t - 2 * pair
    return t, 2 * pair + (1 - core), 2 * (1 - pair) + core


def dot(a, b, over=(1, 0)):
    return lax.dot_general(
        a, b, ((over[:1], over[1:]), ((), ())), preferred_element_type=jnp.float32
    )


def layer_kernel(
    sp_count,
    channels,
    halo,
    routes_ref,
    inner_ref,
    group_ref,
    rstd_ref,
    gain_ref,
    taps_ref,
    norm_ref,
    value_ref,
    gate_in_ref,
    input_hbm,
    cot_hbm,
    gate_hbm,
    up_hbm,
    down_hbm,
    out_proj_hbm,
    gate_out,
    up_out,
    down_out,
    proj_out,
    value_out,
    gate_in_out,
    input_ref,
    cot_ref,
    w_gate,
    w_up,
    w_down,
    out_proj_ref,
    rows_buf,
    pick_buf,
    send_buf,
    slot_buf,
    hidden_buf,
    gate_delta_buf,
    up_delta_buf,
    part_buf,
    mate_buf,
    pair_buf,
    twin_buf,
    total_buf,
    back_buf,
    mixer_ref,
    act_buf,
    slope_buf,
    proj_near,
    proj_own,
    theirs,
    pairs,
    land,
    sums,
    edge,
    ext,
    load_s,
    sp_s,
    sp_r,
    y_s,
    y_r,
    near_s,
    near_r,
    far_s,
    far_r,
    part_s,
    part_r,
    twin_s,
    twin_r,
    back_s,
    back_r,
    ag_s,
    ag_r,
    x_s,
    x_r,
    z_s,
    z_r,
    t_s,
    t_r,
    h_s,
    h_r,
):
    f32, bf16 = jnp.float32, jnp.bfloat16
    me, by_step, _ = ring_peers(sp_count)
    peer = [me] + [by_step[sp_count - mask] for mask in range(1, sp_count)]
    t, mate, twin = tp_places()
    far = 2 * (1 - t // 2) + (mate - 2 * (t // 2))
    tok_rows, model_width = input_ref.shape
    cap = pick_buf.shape[1] // sp_count
    width = model_width // 4
    lanes = 128
    pending = []

    def go(src, dst, sems, index, device):
        copy = remote(src, dst, sems[0].at[index], sems[1].at[index], device)
        copy.start()
        pending.append(copy)

    def arrive(dst, sems, index):
        remote(dst, dst, sems[0].at[index], sems[1].at[index], (me, mate)).wait_recv()

    loads = []
    for i, (src, dst) in enumerate(
        (
            (input_hbm, input_ref),
            (cot_hbm, cot_ref),
            (gate_hbm, w_gate),
            (up_hbm, w_up),
            (down_hbm, w_down),
            (out_proj_hbm, out_proj_ref),
        )
    ):
        copy = pltpu.make_async_copy(src, dst, load_s.at[i])
        copy.start()
        loads.append(copy)
    friends = [(peer[mask], t) for mask in range(1, sp_count)] + [(me, mate), (me, twin), (me, far)]
    barrier = pltpu.get_barrier_semaphore()
    for device in friends:
        pl.semaphore_signal(barrier, inc=1, device_id=device, device_id_type=MESH)

    lane = lax.broadcasted_iota(jnp.int32, (tok_rows, lanes), 1)
    hits = [routes_ref[:, k : k + 1] == lane for k in range(2)]
    both = jnp.where(hits[0] | hits[1], 1.0, 0.0).astype(bf16)
    earlier = jnp.where(
        lax.broadcasted_iota(jnp.int32, (tok_rows, tok_rows), 1)
        < lax.broadcasted_iota(jnp.int32, (tok_rows, tok_rows), 0),
        1.0,
        0.0,
    ).astype(bf16)
    place = dot(earlier, both) + (lane * cap).astype(f32)
    slot = [jnp.sum(jnp.where(hit, place, 0.0), axis=1, keepdims=True) for hit in hits]
    packed = jnp.where(
        lane == 0,
        slot[0],
        jnp.where(
            lane == 1,
            slot[1],
            jnp.where(lane == 2, inner_ref[:, 0:1], jnp.where(lane == 3, inner_ref[:, 1:2], 0.0)),
        ),
    )
    rows_buf[...] = packed.T[0:8]
    pl.semaphore_wait(barrier, len(friends))

    def selection(block):
        ids = (lax.broadcasted_iota(jnp.int32, (cap, tok_rows), 0) + block * cap).astype(f32)
        return ids == rows_buf[0:1, :], ids == rows_buf[1:2, :]

    def chosen(a, hit, columns):
        select = jnp.where(hit[0] | hit[1], 1.0, 0.0).astype(bf16)
        rows = dot(select, (input_ref, cot_ref)[a][:, columns])
        if a == 1:
            scale = jnp.where(hit[0], group_ref[...] * rows_buf[2:3, :], 0.0) + jnp.where(
                hit[1], group_ref[...] * rows_buf[3:4, :], 0.0
            )
            rows = rows * jnp.sum(scale, axis=1, keepdims=True)
        return rows.astype(bf16)

    def spot(a, block, quarter):
        return slot_buf.at[a, rows_of(block, cap), rows_of(quarter, width)]

    order = list(range(1, sp_count))
    for mask in order:
        hit = selection(peer[mask])
        for a in range(2):
            if mask == order[0]:
                loads[a].wait()
            send_buf[a, rows_of(peer[mask], cap)] = chosen(a, hit, rows_of(t, width))
            go(
                send_buf.at[a, rows_of(peer[mask], cap)],
                spot(a, me, t),
                (sp_s, sp_r),
                (a, mask - 1),
                (peer[mask], t),
            )
    hit = selection(me)
    for a in range(2):
        slot_buf[a, rows_of(me, cap)] = chosen(a, hit, pl.ds(0, model_width))

    def expert(mask):
        rows = rows_of(peer[mask], cap)
        slot_input, slot_grad = slot_buf[0, rows], slot_buf[1, rows]
        gate_pre = dot(slot_input, w_gate[...])
        up_pre = dot(slot_input, w_up[...])
        act_grad = dot(slot_grad, w_down[...], (1, 1))
        gate_sigma = jax.nn.sigmoid(gate_pre)
        hidden_buf[rows] = (gate_pre * gate_sigma * up_pre).astype(bf16)
        gate_delta = (act_grad * up_pre * silu_slope(gate_pre, gate_sigma)).astype(bf16)
        up_delta = (act_grad * gate_pre * gate_sigma).astype(bf16)
        gate_delta_buf[rows] = gate_delta
        up_delta_buf[rows] = up_delta
        part_buf[rows] = (
            dot(gate_delta, w_gate[...], (1, 1)) + dot(up_delta, w_up[...], (1, 1))
        ).astype(bf16)
        for j, quarter in ((0, far), (1, mate)):
            go(
                part_buf.at[rows, rows_of(quarter, width)],
                mate_buf.at[j, rows],
                (part_s, part_r),
                (j, mask),
                (me, mate),
            )

    def forward(mask):
        for a in range(2):
            block = spot(a, peer[mask], t)
            arrive(block, (sp_s, sp_r), (a, mask - 1))
            go(block, block, (y_s, y_r), (a, mask - 1), (me, twin))
            go(block, block, (near_s, near_r), (a, mask - 1), (me, mate))

    def across(mask):
        for a in range(2):
            block = spot(a, peer[mask], twin)
            arrive(block, (y_s, y_r), (a, mask - 1))
            go(block, block, (far_s, far_r), (a, mask - 1), (me, mate))

    def work(mask):
        for a in range(2):
            arrive(spot(a, peer[mask], mate), (near_s, near_r), (a, mask - 1))
            arrive(spot(a, peer[mask], far), (far_s, far_r), (a, mask - 1))
        expert(mask)

    def halve(mask):
        rows = rows_of(peer[mask], cap)
        for j, quarter in ((0, twin), (1, t)):
            arrive(mate_buf.at[j, rows], (part_s, part_r), (j, mask))
            pair_buf[j, rows] = (
                part_buf[rows, rows_of(quarter, width)].astype(f32) + mate_buf[j, rows].astype(f32)
            ).astype(bf16)
            if j == 0:
                go(pair_buf.at[0, rows], twin_buf.at[rows], (twin_s, twin_r), mask, (me, twin))

    def give(mask):
        rows = rows_of(peer[mask], cap)
        arrive(twin_buf.at[rows], (twin_s, twin_r), mask)
        total = (pair_buf[1, rows].astype(f32) + twin_buf[rows].astype(f32)).astype(bf16)
        if mask:
            total_buf[rows] = total
            go(
                total_buf.at[rows],
                back_buf.at[rows_of(me, cap)],
                (back_s, back_r),
                mask - 1,
                (peer[mask], t),
            )
        else:
            back_buf[rows] = total

    ids = lax.broadcasted_iota(jnp.int32, pick_buf.shape, 1).astype(f32)
    pick_buf[...] = jnp.where((ids == slot[0]) | (ids == slot[1]), 1.0, 0.0).astype(bf16)
    norm = norm_ref[...].astype(f32)
    normed = norm * gain_ref[...]
    norm_sigma = jax.nn.sigmoid(normed)
    act_buf[...] = (normed * norm_sigma).astype(bf16)
    slope_buf[...] = silu_slope(normed, norm_sigma) * gain_ref[...]
    for i in range(2, 6):
        loads[i].wait()
    forward(order[0])
    expert(0)
    count = len(order)
    for step in range(1, count + 2):
        if step < count:
            forward(order[step])
        if step - 1 < count:
            across(order[step - 1])
        if step - 2 >= 0:
            work(order[step - 2])
        halve(order[step - 3] if step >= 3 else 0) if step != 1 else None
        if step >= 3:
            give(order[step - 4] if step >= 4 else 0)
    down_out[...] = dot(hidden_buf[...], slot_buf[1], (0, 0)).astype(bf16)
    halve(order[-1])
    give(order[-2])
    gate_out[...] = dot(slot_buf[0], gate_delta_buf[...], (0, 0)).astype(bf16)
    give(order[-1])
    up_out[...] = dot(slot_buf[0], up_delta_buf[...], (0, 0)).astype(bf16)
    for mask in order:
        arrive(back_buf.at[rows_of(peer[mask], cap)], (back_s, back_r), mask - 1)

    half = width // 2
    side = lax.rem(me, 2)
    depth = me // 2
    quarters = (t, mate, twin, far)

    def piece(quarter, j):
        return mixer_ref.at[:, rows_of(2 * quarter + j, half)]

    for j in range(2):
        mixed = dot(pick_buf[...], back_buf[:, j * half : (j + 1) * half])
        columns = rows_of(2 * t + j, half)
        mixer_ref[:, columns] = (cot_ref[:, columns].astype(f32) + mixed).astype(bf16)
        go(piece(t, j), piece(t, j), (ag_s, ag_r), (0, j), (me, twin))
        go(piece(t, j), piece(t, j), (ag_s, ag_r), (1, j), (me, mate))

    silu_grad = []

    def project(i):
        quarter = quarters[i]
        near = 2 * quarter + 1 - side
        proj_near[i] = dot(mixer_ref[:, rows_of(near, half)], act_buf[...], (0, 0)).astype(bf16)
        go(proj_near.at[i], theirs.at[i], (x_s, x_r), i, (peer[1], t))
        own = 2 * quarter + side
        proj_own[i] = dot(mixer_ref[:, rows_of(own, half)], act_buf[...], (0, 0))
        silu_grad.append(
            dot(mixer_ref[:, rows_of(quarter, width)], out_proj_ref[rows_of(quarter, width), :])
        )

    def onward(i):
        arrive(theirs.at[i], (x_s, x_r), i)
        pairs[i] = (proj_own[i] + theirs[i].astype(f32)).astype(bf16)
        goal = quarters[i]

        @pl.when(goal != depth)
        def _():
            remote(
                pairs.at[i], land.at[depth], z_s.at[i], z_r.at[depth], (2 * goal + side, t)
            ).start()

    project(0)
    for j in range(2):
        arrive(piece(mate, j), (ag_s, ag_r), (1, j))
    project(1)
    onward(0)
    for j in range(2):
        arrive(piece(twin, j), (ag_s, ag_r), (0, j))
        go(piece(twin, j), piece(twin, j), (ag_s, ag_r), (2, j), (me, mate))
    project(2)
    onward(1)
    for j in range(2):
        arrive(piece(far, j), (ag_s, ag_r), (2, j))
    project(3)
    hat = ((silu_grad[0] + silu_grad[1]) + (silu_grad[2] + silu_grad[3])) * slope_buf[...]
    first = jnp.sum(hat, axis=1, keepdims=True)
    second = jnp.sum(hat * norm, axis=1, keepdims=True)
    sums[0] = jnp.where(lane == 0, first, jnp.where(lane == 1, second, 0.0)).T[0:8]
    for i in range(1, 4):
        go(sums.at[0], sums.at[i], (t_s, t_r), i - 1, (me, quarters[i]))
    onward(2)
    for i in range(1, 4):
        arrive(sums.at[i], (t_s, t_r), i - 1)
    total = (sums[0] + sums[1]) + (sums[2] + sums[3])
    row = lax.broadcasted_iota(jnp.int32, (lanes, tok_rows), 0)
    turned = jnp.where(
        row == 0,
        total[0:1],
        jnp.where(row == 1, total[1:2], jnp.where(row == 2, rstd_ref[...], 0.0)),
    ).T
    conv = turned[:, 2:3] * (
        hat - turned[:, 0:1] / channels - norm * (turned[:, 1:2] / channels)
    )
    edge[0] = conv[:halo]
    previous = lax.rem(me + sp_count - 1, sp_count)
    copy = remote(edge.at[0], edge.at[1], h_s, h_r, (previous, t))
    copy.start()
    pending.append(copy)
    onward(3)
    ext[pl.ds(0, tok_rows)] = conv
    input_sigma = jax.nn.sigmoid(gate_in_ref[...].astype(f32))
    copy.wait_recv()
    ext[pl.ds(tok_rows, halo)] = jnp.where(me == sp_count - 1, 0.0, edge[1])
    tap_count = taps_ref.shape[0]
    taps = taps_ref[...].astype(f32)
    glu = jnp.zeros_like(conv)
    for offset in range(tap_count):
        lower = tap_count - 1 - offset
        glu = glu + taps[offset : offset + 1, :] * ext[pl.ds(lower, tok_rows)]
    value_out[...] = (glu * input_sigma).astype(bf16)
    gate_in_out[...] = (
        glu * value_ref[...].astype(f32) * input_sigma * (1.0 - input_sigma)
    ).astype(bf16)

    own = lax.rem(depth + 0 * t, 4)
    spot_of = 0
    for i in range(4):
        spot_of = spot_of + jnp.where(quarters[i] == own, i, 0)
    total = proj_own[spot_of] + theirs[spot_of].astype(f32)
    for k in range(1, 4):
        other = (depth // 2 + k // 2) % 2 * 2 + (depth + k) % 2
        remote(land.at[other], land.at[other], z_s.at[0], z_r.at[other], (peer[1], t)).wait_recv()
        total = total + land[other].astype(f32)
    proj_out[...] = total
    for i in range(4):

        @pl.when(quarters[i] != depth)
        def _():
            remote(pairs.at[i], land.at[0], z_s.at[i], z_r.at[0], (peer[1], t)).wait_send()

    for copy in pending:
        copy.wait_send()


def by_kernels(
    moe_input,
    out_cotangent,
    routes,
    group_weight,
    inner_weight,
    gate_weight,
    up_weight,
    down_weight,
    value_in,
    gate_in,
    conv_taps,
    norm_hat,
    norm_rstd,
    norm_gain,
    out_proj,
):
    f32, bf16 = jnp.float32, jnp.bfloat16
    tok_rows, model_width = moe_input.shape
    sp_count = lax.axis_size("sp")
    tp_count = lax.axis_size("tp")
    slots = 3 * tok_rows
    width = model_width // tp_count
    hidden = gate_weight.shape[2]
    local = norm_hat.shape[1]
    share = model_width // sp_count
    halo = -(-(conv_taps.shape[0] - 1) // 8) * 8
    dma = pltpu.SemaphoreType.DMA
    vmem = pl.BlockSpec(memory_space=pltpu.VMEM)
    peers = sp_count - 1

    def pair(*shape):
        return [dma(shape), dma(shape)]

    outs = pl.pallas_call(
        functools.partial(layer_kernel, sp_count, local * tp_count, halo),
        out_shape=[
            jax.ShapeDtypeStruct((model_width, hidden), bf16),
            jax.ShapeDtypeStruct((model_width, hidden), bf16),
            jax.ShapeDtypeStruct((hidden, model_width), bf16),
            jax.ShapeDtypeStruct((share, local), f32),
            jax.ShapeDtypeStruct((tok_rows, local), bf16),
            jax.ShapeDtypeStruct((tok_rows, local), bf16),
        ],
        in_specs=[vmem] * 9 + [pl.BlockSpec(memory_space=pl.ANY)] * 6,
        out_specs=[vmem] * 6,
        scratch_shapes=[
            pltpu.VMEM((tok_rows, model_width), bf16),
            pltpu.VMEM((tok_rows, model_width), bf16),
            pltpu.VMEM((model_width, hidden), bf16),
            pltpu.VMEM((model_width, hidden), bf16),
            pltpu.VMEM((hidden, model_width), bf16),
            pltpu.VMEM((model_width, local), bf16),
            pltpu.VMEM((8, tok_rows), f32),
            pltpu.VMEM((tok_rows, slots), bf16),
            pltpu.VMEM((2, slots, width), bf16),
            pltpu.VMEM((2, slots, model_width), bf16),
            pltpu.VMEM((slots, hidden), bf16),
            pltpu.VMEM((slots, hidden), bf16),
            pltpu.VMEM((slots, hidden), bf16),
            pltpu.VMEM((slots, model_width), bf16),
            pltpu.VMEM((2, slots, width), bf16),
            pltpu.VMEM((2, slots, width), bf16),
            pltpu.VMEM((slots, width), bf16),
            pltpu.VMEM((slots, width), bf16),
            pltpu.VMEM((slots, width), bf16),
            pltpu.VMEM((tok_rows, model_width), bf16),
            pltpu.VMEM((tok_rows, local), bf16),
            pltpu.VMEM((tok_rows, local), f32),
            pltpu.VMEM((4, share, local), bf16),
            pltpu.VMEM((4, share, local), f32),
            pltpu.VMEM((4, share, local), bf16),
            pltpu.VMEM((4, share, local), bf16),
            pltpu.VMEM((4, share, local), bf16),
            pltpu.VMEM((4, 8, tok_rows), f32),
            pltpu.VMEM((2, halo, local), f32),
            pltpu.VMEM((tok_rows + halo, local), f32),
            dma((6,)),
        ]
        + pair(2, peers)
        + pair(2, peers)
        + pair(2, peers)
        + pair(2, peers)
        + pair(2, sp_count)
        + pair(sp_count)
        + pair(peers)
        + pair(3, 2)
        + pair(4)
        + pair(4)
        + pair(3)
        + [dma, dma],
        compiler_params=pltpu.CompilerParams(collective_id=1, has_side_effects=True),
        name="layer",
    )(
        routes,
        inner_weight,
        group_weight[None, :],
        norm_rstd[None, :],
        norm_gain[None, :],
        conv_taps,
        norm_hat,
        value_in,
        gate_in,
        moe_input,
        out_cotangent,
        gate_weight[0],
        up_weight[0],
        down_weight[0],
        out_proj,
    )
    return (outs[0][None], outs[1][None], outs[2][None], outs[3], outs[4], outs[5])


def on_device(*arrays):
    tok_rows, model_width = arrays[0].shape
    sp_count, tp_count = lax.axis_size("sp"), lax.axis_size("tp")
    cap = 3 * tok_rows // sp_count
    whole = sp_count == 2 * tp_count and cap % 32 == 0 and model_width // sp_count % 128 == 0
    if whole and tp_count == 4 and arrays[5].shape[0] == 1 and arrays[10].shape[0] > 1:
        return by_kernels(*arrays)
    return by_collectives(*arrays)


def solution(mesh):
    return jax.shard_map(
        on_device,
        mesh=mesh,
        in_specs=(
            P("sp", None),
            P("sp", None),
            P("sp", None),
            P("sp"),
            P("sp", None),
            P("sp", None, "tp"),
            P("sp", None, "tp"),
            P("sp", "tp", None),
            P("sp", "tp"),
            P("sp", "tp"),
            P(None, "tp"),
            P("sp", "tp"),
            P("sp"),
            P("tp"),
            P(None, "tp"),
        ),
        out_specs=(
            P("sp", None, "tp"),
            P("sp", None, "tp"),
            P("sp", "tp", None),
            P("sp", "tp"),
            P("sp", "tp"),
            P("sp", "tp"),
        ),
        check_vma=False,
    )
```
